32 devices in a mesh: rep: 4 (over z), fs: 2 (over y), tp: 4 (over x, core).
Axes of the slice: x: 2, y: 2, z: 4, core: 2. Of those that a mesh axis runs over, the one named last changes fastest.
Arguments:
- inputs: bfloat16 [2560, 2048], P('rep', 'fs'), may hold values from -6 to 6
- gate_pre: bfloat16 [2560, 5632], P('rep', 'tp'), may hold values from -12 to 12
- up_pre: bfloat16 [2560, 5632], P('rep', 'tp'), may hold values from -6 to 6
- cotangent: bfloat16 [2560, 2048], P('rep'), may hold values from -6 to 6
- w_gate: bfloat16 [2048, 5632], P('fs', 'tp'), may hold values from -0.125 to 0.125
- w_up: bfloat16 [2048, 5632], P('fs', 'tp'), may hold values from -0.125 to 0.125
- w_down: bfloat16 [5632, 2048], P('tp', 'fs'), may hold values from -0.078125 to 0.078125
Outputs:
- grad_input: bfloat16 [2560, 2048], P('rep', 'fs')
- grad_gate: float32 [512, 4, 5632], P('fs', 'rep', 'tp')
- grad_up: float32 [512, 4, 5632], P('fs', 'rep', 'tp')
- grad_down: float32 [5632, 512, 4], P('tp', 'fs', 'rep')
- gate_norms: float32 [512, 4], P('fs', 'rep')
- up_norms: float32 [512, 4], P('fs', 'rep')
- down_norms: float32 [5632], P('tp')
The draws below stay inside these ranges and needn't reach their ends.
All inputs are finite; a program needn't handle non-finite values.
Results may differ from the reference program's by a relative error of at most 0.02.
Values may be sent and summed in bfloat16 or wider, within the bound.
No kernel may reach another device: no remote copies, remote signals or barrier semaphores. Data moves between devices by JAX's collectives and lax.ppermute only.
A program may use at most 64 MiB of HBM per device.

```python
import jax
import jax.numpy as jnp
from jax import lax

D = 2048
FF = 5632
TOKENS = 2560
N_REP = 4
N_TP = 4


def raised(values, key, source, target, shards_of, factor):
    def block_of(position):
        return (jnp.arange(values.shape[position]) // (values.shape[position] // shards_of)).reshape((-1,) + (1,) * (values.ndim - 1 - position))

    first = jax.random.permutation(key, shards_of)[block_of(target)]
    far = (block_of(target) + shards_of // 2) % shards_of
    return jnp.where((block_of(source) == first) | (block_of(source) == far), factor * values, values)


def level_of(own_key, shape, pieces, smallest, high):
    def one(dim, blocks):
        heights = jax.random.uniform(jax.random.fold_in(jax.random.fold_in(own_key, 6), dim), (blocks,), jnp.float32, smallest / len(pieces), high / len(pieces))
        return jnp.repeat(jnp.exp(heights), shape[dim] // blocks).reshape((-1,) + (1,) * (len(shape) - dim - 1))

    level = one(*pieces[0])
    for cut in pieces[1:]:
        level = level * one(*cut)
    return level


def bell_draw(own_key, shape, scale, bound, shards=(), kind=jnp.bfloat16):
    loudness = level_of(own_key, shape, shards, -0.22, 0.18) if shards else 1.0
    drawn = jax.random.normal(own_key, shape, jnp.float32) * scale * loudness
    return jnp.minimum(jnp.maximum(drawn, -bound), bound).astype(kind)


def heavy_noise(key, extent, deviation, most, pieces, heavy, held_as=jnp.bfloat16):
    entries = deviation * jax.random.normal(key, extent, jnp.float32)
    if pieces:
        entries = entries * level_of(key, extent, pieces, -0.22, 0.18)
    return jnp.clip(raised(entries, jax.random.fold_in(key, 3), *heavy), -most, most).astype(held_as)


def setup_inputs(seed: int = 0) -> dict:
    streams_of = jax.random.split(jax.random.key(seed), 8)
    return {
        "inputs": bell_draw(streams_of[0], (TOKENS, D), 1.0, 6.0, ((0, 4), (1, 2))),
        "gate_pre": bell_draw(streams_of[1], (TOKENS, FF), 2.0, 12.0, ((0, 4), (1, 4))),
        "up_pre": bell_draw(streams_of[2], (TOKENS, FF), 1.0, 6.0, ((0, 4), (1, 4))),
        "cotangent": heavy_noise(streams_of[3], (TOKENS, D), 1.0, 6.0, ((0, 4),), (0, 1, 4, 2.0)),
        "w_gate": bell_draw(streams_of[4], (D, FF), D ** -0.5, 0.125, ((0, 2), (1, 4))),
        "w_up": bell_draw(streams_of[5], (D, FF), D ** -0.5, 0.125, ((0, 2), (1, 4))),
        "w_down": bell_draw(streams_of[6], (FF, D), FF ** -0.5, 0.078125, ((0, 4), (1, 2))),
    }


def reference(inputs, gate_pre, up_pre, cotangent, w_gate, w_up, w_down):
    single = jnp.float32
    hidden_grad = jnp.dot(cotangent, w_down.T, preferred_element_type=single)
    gate = gate_pre.astype(single)
    upper = up_pre.astype(single)
    sigma = jax.nn.sigmoid(gate)
    active = gate * sigma
    hidden = (active * upper).astype(jnp.bfloat16)
    d_up = (hidden_grad * active).astype(jnp.bfloat16)
    d_gate = (hidden_grad * upper * sigma * (1.0 + gate * (1.0 - sigma))).astype(jnp.bfloat16)
    factor = float(TOKENS) ** -0.5
    grad_gate = jnp.dot(inputs.T, d_gate, preferred_element_type=single) * factor
    grad_up = jnp.dot(inputs.T, d_up, preferred_element_type=single) * factor
    grad_down = jnp.dot(hidden.T, cotangent, preferred_element_type=single) * factor
    block = FF // N_TP
    total = jnp.zeros(inputs.shape, single)
    for index in range(N_TP):
        lower = index * block
        term = jnp.dot(d_gate[:, lower:lower + block], w_gate[:, lower:lower + block].T, preferred_element_type=single)
        term = term + jnp.dot(d_up[:, lower:lower + block], w_up[:, lower:lower + block].T, preferred_element_type=single)
        term = lax.optimization_barrier(term.astype(jnp.bfloat16)).astype(single)
        total = total + term
    grad_input = total.astype(jnp.bfloat16)
    gate_norms = jnp.sum(grad_gate * grad_gate, axis=1).reshape(D // N_REP, N_REP)
    up_norms = jnp.sum(grad_up * grad_up, axis=1).reshape(D // N_REP, N_REP)
    down_norms = jnp.sum(grad_down * grad_down, axis=1)
    return (grad_input, grad_gate.reshape(D // N_REP, N_REP, FF), grad_up.reshape(D // N_REP, N_REP, FF),
            grad_down.reshape(FF, D // N_REP, N_REP), gate_norms, up_norms, down_norms)
```

```python
import functools

import jax
import jax.numpy as jnp
from jax import lax
from jax.experimental import pallas as pl
from jax.experimental.pallas import tpu as pltpu
from jax.sharding import PartitionSpec as P


LANES = 128
SINGLE = jnp.float32
HALF = jnp.bfloat16

OUTER = [(0, 1), (3, 2)]
MIDDLE = [(1, 2), (2, 1)]
INNER = [(1, 0), (2, 3)]

TERMS_BYTES = 28 << 20
FINISH_BYTES = 14 << 20

VMEM = pl.BlockSpec(memory_space=pltpu.VMEM)
SMEM = pl.BlockSpec(memory_space=pltpu.SMEM)
ANY = pl.BlockSpec(memory_space=pl.ANY)


def wide(value):
    return value.astype(SINGLE)


def added(one, other):
    return (wide(one) + wide(other)).astype(HALF)


def to_all(values, axis):
    size = lax.axis_size(axis)
    return [values] + [
        lax.ppermute(values, axis, [(i, i ^ distance) for i in range(size)])
        for distance in range(1, size)
    ]


def regroup(flipped, values, lhs, chunks):
    side = 2 * LANES
    part = side // 4
    owned = lhs.shape[0] // len(chunks)
    target = lax.broadcasted_iota(jnp.int32, (part, side), 0)
    source = lax.broadcasted_iota(jnp.int32, (part, side), 1)
    chosen = []
    for chunk in chunks:
        column = jnp.where(flipped == 1, 3 - chunk, chunk)
        chosen.append((source == target * 4 + column).astype(HALF))
    chosen = jnp.concatenate(chosen, axis=0)
    for index in range(values.shape[1] // side):
        picked = lax.dot_general(
            chosen,
            values[:, index * side:(index + 1) * side],
            (((1,), (1,)), ((), ())),
            preferred_element_type=SINGLE,
        ).astype(HALF)
        for b in range(len(chunks)):
            lhs[b * owned + index * part:b * owned + (index + 1) * part, :] = picked[b * part:(b + 1) * part]


def terms_kernel(factor, grads, halves, order, where, features, gates, ups, *rest):
    *rest, lhs, deltas = rest
    if halves:
        *rest, half_out = rest
    if grads:
        partial, other, *outs, gate_out, up_out = rest
    else:
        outs = rest
    owned = lhs.shape[0] // len(order)
    units = gates.shape[1]
    step = pl.program_id(0)
    now = lax.rem(step, 2)

    @pl.when(step == 0)
    def _():
        regroup(where[0], features, lhs, order)

    def products():
        value = jnp.dot(lhs[...], deltas[1 - now], preferred_element_type=SINGLE) * factor
        value = value.astype(HALF)
        for place, out in enumerate(outs):
            rows = value[place * owned:(place + 1) * owned]
            if grads:
                for which in range(2):
                    out[which] = rows[:, which * units:(which + 1) * units]
            else:
                out[...] = rows

    def factors():
        gate = wide(gates[...])
        upper = wide(ups[...])
        sigma = 0.5 * jnp.tanh(0.5 * gate) + 0.5
        active = gate * sigma
        if grads:
            hidden_grad = wide(partial[...]) + wide(other[...])
            d_up = (hidden_grad * active).astype(HALF)
            d_gate = (hidden_grad * upper * sigma * (1.0 + gate * (1.0 - sigma))).astype(HALF)
            gate_out[...] = d_gate
            up_out[...] = d_up
            deltas[now, :, :units] = d_gate
            deltas[now, :, units:] = d_up
            if halves:
                count = half_out.shape[1]
                chosen = pl.ds(pl.multiple_of(where[2] * count, 16), count)
                half_out[0] = gate_out[chosen, :]
                half_out[1] = up_out[chosen, :]
        else:
            deltas[now] = (active * upper).astype(HALF)

    products()
    factors()


def terms(where, features, width, gate_pre, up_pre, factor, order, span, units, grads=None, halves=False):
    tokens = gate_pre.shape[0]
    low, hunits = span[0], span[1] - span[0]
    owned = width // 4
    steps = -(-hunits // units)
    here = pl.BlockSpec((tokens, units), lambda j, _: (0, jnp.minimum(j, steps - 1)))
    saved = pl.BlockSpec((tokens, units), lambda j, _: (0, low // units + jnp.minimum(j, steps - 1)))
    if grads:
        out = [pl.BlockSpec((2, owned, units), lambda j, _: (0, 0, jnp.maximum(j - 1, 0)))] * len(order) + [here, here]
        shapes = [jax.ShapeDtypeStruct((2, owned, hunits), HALF)] * len(order)
        shapes += [jax.ShapeDtypeStruct((tokens, hunits), HALF)] * 2
        if halves:
            out.append(pl.BlockSpec((2, tokens // 2, units), lambda j, _: (0, 0, jnp.minimum(j, steps - 1))))
            shapes.append(jax.ShapeDtypeStruct((2, tokens // 2, hunits), HALF))
    else:
        out = [pl.BlockSpec((owned, units), lambda j, _: (0, jnp.maximum(j - 1, 0)))] * len(order)
        shapes = [jax.ShapeDtypeStruct((owned, hunits), HALF)] * len(order)
    products = 2 if grads else 1
    rows = owned * len(order)
    return pl.pallas_call(
        functools.partial(terms_kernel, factor, bool(grads), halves, order),
        grid_spec=pltpu.PrefetchScalarGridSpec(
            num_scalar_prefetch=1,
            grid=(steps + 1,),
            in_specs=[pl.BlockSpec((tokens, width), lambda j, where: (0, where[1])), saved, saved]
            + ([here, here] if grads else []),
            out_specs=out,
            scratch_shapes=[
                pltpu.VMEM((rows, tokens), HALF),
                pltpu.VMEM((2, tokens, products * units), HALF),
            ],
        ),
        out_shape=shapes,
        compiler_params=pltpu.CompilerParams(vmem_limit_bytes=TERMS_BYTES),
        cost_estimate=pl.CostEstimate(
            flops=2 * tokens * rows * hunits * products,
            bytes_accessed=2 * (tokens * width + rows * hunits * products + 4 * tokens * hunits),
            transcendentals=tokens * hunits,
        ),
    )(where, features, gate_pre, up_pre, *(grads or ()))


def first_kernel(factor, order, where, features, gates_all, ups_all, out, buffer, gates, ups, lhs, deltas, sems):
    tokens, hunits = gates.shape
    width = buffer.shape[1]
    rows = tokens // 4
    units = 2 * LANES
    blocks = [pl.ds(low, min(units, hunits - low)) for low in range(0, hunits, units)]
    start = pl.multiple_of(where[1] * width, LANES)
    early = [
        pltpu.make_async_copy(
            features.at[pl.ds(k * rows, rows), pl.ds(start, width)], buffer.at[pl.ds(k * rows, rows)], sems.at[k])
        for k in range(4)
    ]
    pairs = [
        [
            pltpu.make_async_copy(source.at[:, block], target.at[:, block], sems.at[4 + 2 * k + which])
            for which, (source, target) in enumerate(((gates_all, gates), (ups_all, ups)))
        ]
        for k, block in enumerate(blocks)
    ]
    for copy in early:
        copy.start()
    for pair in pairs:
        for copy in pair:
            copy.start()
    for copy in early:
        copy.wait()
    regroup(where[0], buffer, lhs, order)
    for k, (block, pair) in enumerate(zip(blocks, pairs)):
        for copy in pair:
            copy.wait()
        gate = wide(gates[:, block])
        hidden = gate * (0.5 * jnp.tanh(0.5 * gate) + 0.5) * wide(ups[:, block])
        deltas[k % 2, :, :block.size] = hidden.astype(HALF)
        value = jnp.dot(lhs[...], deltas[k % 2, :, :block.size], preferred_element_type=SINGLE) * factor
        out[:, block] = value.astype(HALF)


def first_terms(where, features, width, gate_pre, up_pre, factor, order):
    tokens, hunits = gate_pre.shape
    owned = width // 4
    return pl.pallas_call(
        functools.partial(first_kernel, factor, order),
        in_specs=[SMEM, ANY, ANY, ANY],
        out_specs=VMEM,
        out_shape=jax.ShapeDtypeStruct((owned, hunits), HALF),
        scratch_shapes=[
            pltpu.VMEM((tokens, width), HALF),
            pltpu.VMEM((tokens, hunits), HALF),
            pltpu.VMEM((tokens, hunits), HALF),
            pltpu.VMEM((owned, tokens), HALF),
            pltpu.VMEM((2, tokens, 2 * LANES), HALF),
            pltpu.SemaphoreType.DMA((4 + 2 * -(-hunits // (2 * LANES)),)),
        ],
        cost_estimate=pl.CostEstimate(
            flops=2 * tokens * owned * hunits,
            bytes_accessed=2 * (tokens * width + owned * hunits + 2 * tokens * hunits),
            transcendentals=tokens * hunits,
        ),
    )(where, features, gate_pre, up_pre)


def extend_kernel(factor, order, where, *refs):
    quarters, (came, shared), own, outs = refs[:4], refs[4:6], refs[6:9], refs[9:12]
    features, deltas, lhs = refs[12:]
    rows = quarters[0].shape[0]
    for distance, quarter in enumerate(quarters):
        place = jnp.bitwise_xor(where[3], distance)
        features[pl.ds(pl.multiple_of(place * rows, 16), rows), :] = quarter[...]
    count = came.shape[1]
    for half, value in ((where[2], came), (1 - where[2], shared)):
        deltas[:, pl.ds(pl.multiple_of(half * count, 16), count), :] = value[...]
    regroup(where[0], features, lhs, order)
    owned = lhs.shape[0] // len(order)
    units = came.shape[2]
    for which in range(2):
        for low in range(0, units, 2 * LANES):
            block = pl.ds(low, min(2 * LANES, units - low))
            value = jnp.dot(lhs[...], deltas[which, :, block], preferred_element_type=SINGLE) * factor
            for place in range(len(order)):
                total = value[place * owned:(place + 1) * owned] + wide(own[place][which, :, block])
                outs[place][which, :, block] = total.astype(HALF)


def extend(where, quarters, halves, own, factor, order):
    rows, width = quarters[0].shape
    units = halves[0].shape[2]
    tokens = 2 * halves[0].shape[1]
    return pl.pallas_call(
        functools.partial(extend_kernel, factor, order),
        in_specs=[SMEM] + [VMEM] * 9,
        out_specs=[VMEM] * 3,
        out_shape=[jax.ShapeDtypeStruct(own[0].shape, HALF)] * 3,
        scratch_shapes=[
            pltpu.VMEM((4 * rows, width), HALF),
            pltpu.VMEM((2, tokens, units), HALF),
            pltpu.VMEM((width // 4 * 3, tokens), HALF),
        ],
        compiler_params=pltpu.CompilerParams(vmem_limit_bytes=TERMS_BYTES),
        cost_estimate=pl.CostEstimate(
            flops=3 * tokens * width * units,
            bytes_accessed=2 * (tokens * width + 2 * tokens * units + 3 * width * units),
            transcendentals=0,
        ),
    )(where, *quarters, *halves, *own)


def fetch(sources, buffers, sems):
    copies = [
        pltpu.make_async_copy(source, buffers.at[k], sems.at[k]) for k, source in enumerate(sources)
    ]
    for copy in copies:
        copy.start()
    for copy in copies:
        copy.wait()


def total_of(flag, parts):
    total = wide(jnp.where(flag[0] == 1, parts[0], parts[1]))
    for part in parts[2:]:
        total = total + wide(part)
    return total


def finish_rows_kernel(low, first, count, flag, *rest):
    parts, rest = rest[:count], rest[count:]
    buffers, stage, sems, out_sems = rest[-4:]
    gate_out, up_out, norms = rest[-7:-4]
    units = stage.shape[3]
    fetch(parts, buffers, sems)
    copies = []
    for which, out in enumerate((gate_out, up_out)):
        value = total_of(flag, [buffers[k, which] for k in range(count)])
        stage[which, :, 0, :] = value
        copy = pltpu.make_async_copy(stage.at[which], out.at[:, :, pl.ds(low, units)], out_sems.at[which])
        copy.start()
        copies.append(copy)
        square = value * value
        lanes = square[:, :LANES]
        for start in range(LANES, units, LANES):
            lanes = lanes + square[:, start:start + LANES]
        total = jnp.sum(lanes.T, axis=0, keepdims=True)
        norms[which:which + 1, :] = total if first else total + rest[2][which:which + 1, :]
    for copy in copies:
        copy.wait()


def finish_columns_kernel(count, flag, *rest):
    parts, (out, norms, buffers, stage, sems, out_sems) = rest[:count], rest[count:]
    fetch(parts, buffers, sems)
    value = total_of(flag, [buffers[k] for k in range(count)])
    stage[:, 0, :] = value.T
    copy = pltpu.make_async_copy(stage, out, out_sems.at[0])
    copy.start()
    norms[...] = jnp.sum(value * value, axis=0, keepdims=True)
    copy.wait()


def finish(flag, parts, low=0, whole=None, before=()):
    *pair, owned, hunits = parts[0].shape
    count = len(parts)
    if pair:
        wholes = [jax.ShapeDtypeStruct((owned, 1, whole), SINGLE)] * 2
        norms, stage = (2, owned), (2, owned, 1, hunits)
        kernel = functools.partial(finish_rows_kernel, low, not before, count)
    else:
        wholes = [jax.ShapeDtypeStruct((hunits, 1, owned), SINGLE)]
        norms, stage = (1, hunits), (hunits, 1, owned)
        kernel = functools.partial(finish_columns_kernel, count)
    return pl.pallas_call(
        kernel,
        in_specs=[SMEM] + [ANY] * count + ([ANY, ANY, VMEM] if before else []),
        out_specs=[ANY] * len(wholes) + [VMEM],
        out_shape=wholes + [jax.ShapeDtypeStruct(norms, SINGLE)],
        scratch_shapes=[
            pltpu.VMEM((count, *parts[0].shape), HALF),
            pltpu.VMEM(stage, SINGLE),
            pltpu.SemaphoreType.DMA((count,)),
            pltpu.SemaphoreType.DMA((2,)),
        ],
        input_output_aliases={count + 1: 0, count + 2: 1} if before else {},
        compiler_params=pltpu.CompilerParams(vmem_limit_bytes=FINISH_BYTES),
        cost_estimate=pl.CostEstimate(
            flops=1_000_000_000, bytes_accessed=owned * hunits * 14, transcendentals=0),
    )(flag, *parts, *before)


def pair_sum_kernel(*refs):
    *parts, one, two = refs
    total = sum(part[...] for part in parts)
    one[...] = total[0:1]
    two[...] = total[1:2]


def on_line(inputs, gate_pre, up_pre, cotangent, w_gate, w_up, w_down):
    return line_body(inputs, gate_pre, up_pre, cotangent, w_gate, w_up, w_down)


def line_body(inputs, gate_pre, up_pre, cotangent, w_gate, w_up, w_down):
    groups = lax.axis_size("rep")
    place = lax.axis_index("rep")
    flipped = place >= groups // 2
    flag = ((place == 0) | (place == groups - 1)).astype(jnp.int32)[None]
    width = w_down.shape[1]
    hunits = w_gate.shape[1]
    factor = float(inputs.shape[0] * groups) ** (-0.5)
    swap = [(0, 1), (1, 0)]

    half = lax.axis_index("fs").astype(jnp.int32)
    flipped = flipped.astype(jnp.int32)
    place = lax.axis_index("tp").astype(jnp.int32)
    of_cot = jnp.stack([flipped, half, half, place])
    of_inputs = jnp.stack([flipped, jnp.zeros_like(half), half, place])

    rows = inputs.shape[0] // 4
    quarter = lax.dynamic_slice_in_dim(inputs, place * rows, rows, 0)
    apart = lambda distance: [(i, i ^ distance) for i in range(4)]
    quarters = {0: lax.ppermute(quarter, "rep", OUTER)}
    quarters[2] = lax.ppermute(quarters[0], "tp", apart(2))
    quarters[1] = lax.ppermute(quarters[0], "tp", apart(1))
    quarters[3] = lax.ppermute(quarters[2], "tp", apart(1))
    quarters = [quarters[distance] for distance in range(4)]

    edge = -(-hunits // (6 * LANES)) * 2 * LANES
    spans = [(0, edge), (2 * edge, hunits), (edge, 2 * edge)]
    partials, others = [], []
    for k, (low, high) in enumerate(spans):
        own_cot = lax.dynamic_slice_in_dim(lax.optimization_barrier(cotangent), half * width, width, 1)
        partial = jnp.einsum("td,fd->tf", own_cot, w_down[low:high], preferred_element_type=SINGLE)
        partials.append(partial.astype(HALF))
        others.append(lax.ppermute(partials[k], "fs", swap))

    def passed(value):
        return lax.ppermute(added(value, lax.ppermute(value, "rep", OUTER)), "rep", MIDDLE)

    far = first_terms(of_cot, cotangent, width, gate_pre, up_pre, factor, (3,))
    near, mine, local = terms(of_cot, cotangent, width, gate_pre, up_pre, factor, (2, 1, 0), (0, hunits), 4 * LANES)
    far_over = passed(far)
    near_over = passed(near)
    came = lax.ppermute(mine, "rep", OUTER)
    back = lax.ppermute(added(local, far_over), "rep", INNER)
    grad_down, squares = finish(flag, (local, mine, near_over, back, came))
    grad_down = jnp.swapaxes(grad_down, 1, 2)
    from_other = lax.ppermute(squares, "fs", swap)
    squares = squares + from_other
    squares = to_all(squares, "rep")
    down_norms = sum(part[0] for part in squares)

    def gradients(k, halves):
        return terms(
            of_inputs, inputs, width, gate_pre, up_pre, factor, (3, 2, 1, 0), spans[k], 2 * LANES,
            (partials[k], others[k]), halves)

    far, near, mine, local0, *first, part = gradients(0, True)
    part = lax.ppermute(part, "rep", OUTER)
    far, near, mine0 = extend(
        of_inputs, quarters, (part, lax.ppermute(part, "fs", swap)), (far, near, mine), factor, (3, 2, 1))
    far_over = lax.ppermute(far, "rep", MIDDLE)
    near_over0 = lax.ppermute(near, "rep", MIDDLE)
    back0 = lax.ppermute(added(local0, far_over), "rep", INNER)

    deltas, sums = [first], []
    for k in (1, 2):
        far, near, mine, local, *more = gradients(k, False)
        deltas.append(more)
        far_over = passed(far)
        near_over = passed(near)
        came = lax.ppermute(mine, "rep", OUTER)
        back = lax.ppermute(added(local, far_over), "rep", INNER)
        sums.append((local, mine, near_over, back, came))
    buffers = finish(flag, sums[0], spans[1][0], hunits)
    buffers = finish(flag, (local0, mine0, near_over0, back0), 0, hunits, buffers)
    grad_gate, grad_up, squares = finish(flag, sums[1], spans[2][0], hunits, buffers)
    squares = to_all(squares, "tp")
    owned = width // groups
    gate_norms, up_norms = pl.pallas_call(
        pair_sum_kernel, out_shape=[jax.ShapeDtypeStruct((1, owned), SINGLE)] * 2,
        compiler_params=pltpu.CompilerParams(vmem_limit_bytes=1 << 20), name="gq")(*squares)
    gate_norms, up_norms = jnp.swapaxes(gate_norms, 0, 1), jnp.swapaxes(up_norms, 0, 1)

    term = None
    for pair, (low, high) in zip(deltas, spans):
        for delta, weight in zip(pair, (w_gate, w_up)):
            one = jnp.einsum("tf,df->td", delta, weight[:, low:high], preferred_element_type=SINGLE)
            term = one if term is None else term + one
    term = term.astype(HALF)
    term = added(term, lax.ppermute(term, "tp", apart(2)))
    grad_input = added(term, lax.ppermute(term, "tp", apart(1)))
    return (
        grad_input,
        grad_gate,
        grad_up,
        grad_down,
        gate_norms,
        up_norms,
        down_norms,
    )


def anywhere(inputs, gate_pre, up_pre, cotangent, w_gate, w_up, w_down):
    groups = lax.axis_size("rep")
    width = w_down.shape[1]
    own_cot = lax.dynamic_slice_in_dim(cotangent, lax.axis_index("fs") * width, width, 1)
    partial_grad = jnp.einsum("td,fd->tf", own_cot, w_down, preferred_element_type=SINGLE)
    hidden_grad = wide(lax.psum(partial_grad.astype(HALF), "fs"))
    gate = wide(gate_pre)
    upper = wide(up_pre)
    sigma = jax.nn.sigmoid(gate)
    active = gate * sigma
    hidden = (active * upper).astype(HALF)
    d_up = (hidden_grad * active).astype(HALF)
    d_gate = (hidden_grad * upper * sigma * (1.0 + gate * (1.0 - sigma))).astype(HALF)
    factor = float(inputs.shape[0] * groups) ** (-0.5)
    owned = width // groups
    hunits = w_gate.shape[1]

    def owner_sum(local, axis):
        parts = lax.all_to_all(local.astype(HALF), "rep", split_axis=axis, concat_axis=axis, tiled=True)
        return jnp.sum(wide(parts), axis=axis, keepdims=True)

    gate_local = jnp.einsum("td,tf->df", inputs, d_gate, preferred_element_type=SINGLE) * factor
    grad_gate = owner_sum(gate_local.reshape(owned, groups, hunits), 1)
    up_local = jnp.einsum("td,tf->df", inputs, d_up, preferred_element_type=SINGLE) * factor
    grad_up = owner_sum(up_local.reshape(owned, groups, hunits), 1)
    down_local = jnp.einsum("tf,td->fd", hidden, own_cot, preferred_element_type=SINGLE) * factor
    grad_down = owner_sum(down_local.reshape(hunits, owned, groups), 2)
    input_term = jnp.einsum("tf,df->td", d_gate, w_gate, preferred_element_type=SINGLE)
    input_term = input_term + jnp.einsum("tf,df->td", d_up, w_up, preferred_element_type=SINGLE)
    grad_input = lax.psum(input_term.astype(HALF), "tp")
    gate_norms, up_norms = lax.psum(
        (jnp.sum(grad_gate * grad_gate, axis=2), jnp.sum(grad_up * grad_up, axis=2)), "tp"
    )
    down_norms = lax.psum(jnp.sum(grad_down * grad_down, axis=(1, 2)), ("rep", "fs"))
    return (grad_input, grad_gate, grad_up, grad_down, gate_norms, up_norms, down_norms)


def solution(mesh):
    placed = (
        P("rep", "fs"),
        P("rep", "tp"),
        P("rep", "tp"),
        P("rep", None),
        P("fs", "tp"),
        P("fs", "tp"),
        P("tp", "fs"),
    )
    line = (mesh.shape["rep"], mesh.shape["fs"], mesh.shape["tp"]) == (4, 2, 4)
    return jax.shard_map(
        on_line if line else anywhere,
        mesh=mesh,
        in_specs=placed,
        out_specs=(
            P("rep", "fs"),
            P("fs", "rep", "tp"),
            P("fs", "rep", "tp"),
            P("tp", "fs", "rep"),
            P("fs", "rep"),
            P("fs", "rep"),
            P("tp"),
        ),
        check_vma=False,
    )
```
